32 devices in a mesh: fs: 8 (over z, core), tp: 4 (over y, x).
Axes of the slice: x: 2, y: 2, z: 4, core: 2. Of those that a mesh axis runs over, the one named last changes fastest.
Arguments:
- in_saved: bfloat16 [6144, 2048], P(('fs', 'tp')), may hold values from -6 to 6
- in_cotangent: bfloat16 [6144, 2048], P(('fs', 'tp')), as said below
- point_saved: bfloat16 [6144, 2048], P(('fs', 'tp')), may hold values from -6 to 6
- point_cotangent: bfloat16 [6144, 2048], P(('fs', 'tp')), as said below
- in_basis: bfloat16 [2048, 128], replicated, as said below
- point_basis: bfloat16 [2048, 128], replicated, as said below
- in_first: float32 [128, 2048], P('fs', 'tp'), may hold values from -3 to 3
- in_second: float32 [128, 2048], P('fs', 'tp'), may hold values from 0.02 to 2
- point_first: float32 [128, 2048], P('fs', 'tp'), may hold values from -3 to 3
- point_second: float32 [128, 2048], P('fs', 'tp'), may hold values from 0.02 to 2
- in_master: float32 [2048, 2048], P('fs', 'tp'), may hold values from -3 to 3
- point_master: float32 [2048, 2048], P('fs', 'tp'), may hold values from -3 to 3
Outputs:
- in_first_new: float32 [128, 2048], P('fs', 'tp')
- in_second_new: float32 [128, 2048], P('fs', 'tp')
- point_first_new: float32 [128, 2048], P('fs', 'tp')
- point_second_new: float32 [128, 2048], P('fs', 'tp')
- in_step: float32 [2048, 2048], P('fs', 'tp')
- point_step: float32 [2048, 2048], P('fs', 'tp')
- in_master_new: float32 [2048, 2048], P('fs', 'tp')
- point_master_new: float32 [2048, 2048], P('fs', 'tp')
- in_copy: bfloat16 [2048, 2048], P(None, 'tp')
- point_copy: bfloat16 [2048, 2048], P(None, 'tp')
The draws below stay inside these ranges and needn't reach their ends.
Inputs may be any that keep to these rules, and one draw needn't show every extreme that they name: `in_cotangent`: real-valued entries of every column. `point_cotangent`: real-valued entries of every column. `in_basis`: real-valued basis of full rank. `point_basis`: real-valued basis of full rank.
All inputs are finite; a program needn't handle non-finite values.
Results may differ from the reference program's by a relative error of at most 0.0034.
Values may be sent and summed in bfloat16 or wider, within the bound.
No kernel may reach another device: no remote copies, remote signals or barrier semaphores. Data moves between devices by JAX's collectives and lax.ppermute only.
A program may use at most 64 MiB of HBM per device.

```python
import math
import jax
import jax.numpy as jnp
from jax import lax

D = 2048
C = 2048
RANK = 128
TOK_DEV = 192
TOKENS = 6144
N_FS = 8
N_TP = 4


def cotangent_draw(key, width):
    keys = jax.random.split(jax.random.fold_in(key, 7), 3)
    offset = jax.random.uniform(keys[1], (width,), jnp.float32)
    levels = (jnp.arange(width).astype(jnp.float32) + offset) / width
    scales = 10.0 ** levels / 3.9
    shift = jax.random.randint(keys[2], (), 0, N_TP)
    device = jnp.arange(TOKENS) // TOK_DEV
    target = (device + shift) % N_TP
    column_block = jnp.arange(width) // (width // N_TP)
    boost = jnp.where(column_block[None, :] == target[:, None], 4.0, 1.0)
    noise = jax.random.truncated_normal(keys[0], -4.0, 4.0, (TOKENS, width), jnp.float32)
    return (noise * scales[None, :] * boost).astype(jnp.bfloat16)


def basis_draw(key, rows):
    keys = jax.random.split(jax.random.fold_in(key, 11), 2)
    offset = jax.random.uniform(keys[1], (RANK,), jnp.float32)
    levels = (jnp.arange(RANK).astype(jnp.float32) + offset) / RANK
    noise = jax.random.truncated_normal(keys[0], -4.0, 4.0, (rows, RANK), jnp.float32)
    scales = 10.0 ** levels
    return (noise * scales[None, :] / (3.9 * jnp.sqrt(rows * 1.0))).astype(jnp.bfloat16)


def draw_in_cotangent(key, part):
    return cotangent_draw(jax.random.fold_in(key, 1), C)


def draw_point_cotangent(key, part):
    return cotangent_draw(jax.random.fold_in(key, 2), D)


def draw_in_basis(key, part):
    return basis_draw(jax.random.fold_in(key, 3), D)


def draw_point_basis(key, part):
    return basis_draw(jax.random.fold_in(key, 4), C)


def shard_levels(rng, dims, cuts, smallest, largest):
    factor_of = 1.0
    for axis_at, parts in cuts:
        draws = jax.random.uniform(jax.random.fold_in(jax.random.fold_in(rng, 6), axis_at), (parts,), jnp.float32, smallest / len(cuts), largest / len(cuts))
        factor_of = factor_of * jnp.repeat(jnp.exp(draws), dims[axis_at] // parts).reshape((-1,) + (1,) * (len(dims) - 1 - axis_at))
    return factor_of


def normal_values(rng, dims, scale, most, shards=(), dtype=jnp.bfloat16):
    values = scale * jax.random.normal(rng, dims, jnp.float32)
    if shards:
        values = values * shard_levels(rng, dims, shards, -0.22, 0.18)
    return jnp.clip(values, -most, most).astype(dtype)


def setup_inputs(seed: int = 0) -> dict:
    seeds = jax.random.split(jax.random.key(seed), 13)
    in_saved = normal_values(seeds[0], (TOKENS, D), 1.0, 6.0, ((0, 32),))
    in_cotangent = draw_in_cotangent(jax.random.fold_in(seeds[12], 71), 0)
    point_saved = normal_values(seeds[2], (TOKENS, C), 1.0, 6.0, ((0, 32),))
    point_cotangent = draw_point_cotangent(jax.random.fold_in(seeds[12], 71), 0)
    in_basis = draw_in_basis(jax.random.fold_in(seeds[12], 71), 0)
    point_basis = draw_point_basis(jax.random.fold_in(seeds[12], 71), 0)
    in_first = normal_values(seeds[6], (RANK, C), 0.5, 3.0, ((0, 8), (1, 4)), jnp.float32)
    in_second = jnp.clip(jnp.exp(math.log(2.0) - 4.6051702 * jax.random.uniform(seeds[7], (RANK, C), jnp.float32) ** shard_levels(seeds[7], (RANK, C), ((0, 8), (1, 4)), -0.2, 0.2)), 0.02, 2.0)
    point_first = normal_values(seeds[8], (RANK, D), 0.5, 3.0, ((0, 8), (1, 4)), jnp.float32)
    point_second = jnp.clip(jnp.exp(math.log(2.0) - 4.6051702 * jax.random.uniform(seeds[9], (RANK, D), jnp.float32) ** shard_levels(seeds[9], (RANK, D), ((0, 8), (1, 4)), -0.2, 0.2)), 0.02, 2.0)
    in_master = normal_values(seeds[10], (D, C), 0.5, 3.0, ((0, 8), (1, 4)), jnp.float32)
    point_master = normal_values(seeds[11], (C, D), 0.5, 3.0, ((0, 8), (1, 4)), jnp.float32)
    return {"in_saved": in_saved, "in_cotangent": in_cotangent, "point_saved": point_saved, "point_cotangent": point_cotangent, "in_basis": in_basis, "point_basis": point_basis, "in_first": in_first, "in_second": in_second, "point_first": point_first, "point_second": point_second, "in_master": in_master, "point_master": point_master}


def low_grad(saved, cotangent, basis):
    basis_f = basis.astype(jnp.float32)
    saved_blocks = saved.reshape(N_FS, -1, saved.shape[1])
    cot_blocks = cotangent.reshape(N_FS, -1, cotangent.shape[1])

    def add_block(total, pair):
        reduced = jnp.dot(pair[0].astype(jnp.float32), basis_f).astype(jnp.bfloat16)
        term = jnp.dot(reduced.astype(jnp.float32).T, pair[1].astype(jnp.float32))
        return (total + term, None)
    start = jnp.zeros((basis.shape[1], cotangent.shape[1]), jnp.float32)
    total, unused = lax.scan(add_block, start, (saved_blocks, cot_blocks))
    return total

def moments(first, second, grad):
    first_new = 0.8 * first + 0.2 * grad
    second_new = 0.9 * second + 0.1 * grad * grad
    return (first_new, second_new, first_new / (jnp.sqrt(second_new) + 1e-08))

def reference(in_saved, in_cotangent, point_saved, point_cotangent, in_basis, point_basis, in_first, in_second, point_first, point_second, in_master, point_master):
    in_low = low_grad(in_saved, in_cotangent, in_basis)
    point_low = low_grad(point_saved, point_cotangent, point_basis)
    entries = 1.0 * in_low.shape[0] * (in_low.shape[1] + point_low.shape[1])
    squares = jnp.sum(in_low * in_low) + jnp.sum(point_low * point_low)
    rms_value = jnp.sqrt(squares / entries + 1e-06)
    clip_factor = jnp.minimum(1.0, 1.0 / rms_value)
    in_first_new, in_second_new, in_direction = moments(in_first, in_second, clip_factor * in_low)
    point_first_new, point_second_new, point_direction = moments(point_first, point_second, clip_factor * point_low)
    in_step = -jnp.dot(in_basis.astype(jnp.float32), in_direction, precision=lax.Precision.HIGHEST)
    point_step = -jnp.dot(point_basis.astype(jnp.float32), point_direction, precision=lax.Precision.HIGHEST)
    in_master_new = in_master + in_step
    point_master_new = point_master + point_step
    return (in_first_new, in_second_new, point_first_new, point_second_new, in_step, point_step, in_master_new, point_master_new, in_master_new.astype(jnp.bfloat16), point_master_new.astype(jnp.bfloat16))
```

```python
import jax
import jax.numpy as jnp
from jax import lax
from jax.experimental import pallas as pl
from jax.experimental.pallas import tpu as pltpu
from jax.sharding import PartitionSpec as P

CORES = 2


def low_term(saved, cotangent, basis):
    reduced = jnp.dot(saved, basis, preferred_element_type=jnp.float32).astype(jnp.bfloat16)
    return lax.dot_general(
        reduced, cotangent, (((0,), (0,)), ((), ())), preferred_element_type=jnp.float32
    )


def moments(first, second, grad):
    first_new = 0.8 * first + 0.2 * grad
    second_new = 0.9 * second + 0.1 * grad * grad
    return (first_new, second_new, first_new / (jnp.sqrt(second_new) + 1e-08))


def weight_step(basis, direction, fs_count):
    row_count = basis.shape[0] // fs_count
    rows_here = lax.dynamic_slice_in_dim(basis, lax.axis_index("fs") * row_count, row_count, 0)
    return -jnp.dot(rows_here.astype(jnp.float32), direction, precision=lax.Precision.HIGHEST)


def clip_of(squares, entries):
    return jnp.minimum(1.0, 1.0 / jnp.sqrt(squares / entries + 1e-06))


def plain_body(
    in_saved,
    in_cotangent,
    point_saved,
    point_cotangent,
    in_basis,
    point_basis,
    in_first,
    in_second,
    point_first,
    point_second,
    in_master,
    point_master,
):
    fs_count = lax.axis_size("fs")
    in_low = low_term(in_saved, in_cotangent, in_basis)
    point_low = low_term(point_saved, point_cotangent, point_basis)
    rank_rows = in_low.shape[0]
    entries = 1.0 * rank_rows * (in_low.shape[1] + point_low.shape[1])
    part_in, part_point = (
        lax.psum_scatter(in_low, "tp", scatter_dimension=1, tiled=True),
        lax.psum_scatter(point_low, "tp", scatter_dimension=1, tiled=True),
    )
    sum_in, sum_point = lax.psum((part_in, part_point), "fs")
    squares = lax.psum(jnp.sum(sum_in * sum_in) + jnp.sum(sum_point * sum_point), "tp")
    clip_factor = clip_of(squares, entries)
    previous = tuple(
        lax.all_gather(a, "fs", axis=0, tiled=True)
        for a in (in_first, in_second, point_first, point_second)
    )
    in_first_all, in_second_all, in_direction = moments(
        previous[0], previous[1], clip_factor * sum_in
    )
    point_first_all, point_second_all, point_direction = moments(
        previous[2], previous[3], clip_factor * sum_point
    )
    row_count = rank_rows // fs_count
    row_start = lax.axis_index("fs") * row_count
    mine = tuple(
        lax.dynamic_slice_in_dim(a, row_start, row_count, 0)
        for a in (in_first_all, in_second_all, point_first_all, point_second_all)
    )
    in_step = weight_step(in_basis, in_direction, fs_count)
    point_step = weight_step(point_basis, point_direction, fs_count)
    in_master_new = in_master + in_step
    point_master_new = point_master + point_step
    in_copy, point_copy = (
        lax.all_gather(in_master_new.astype(jnp.bfloat16), "fs", axis=0, tiled=True),
        lax.all_gather(point_master_new.astype(jnp.bfloat16), "fs", axis=0, tiled=True),
    )
    return (*mine, in_step, point_step, in_master_new, point_master_new, in_copy, point_copy)


def fs_xor(x, mask):
    return lax.ppermute(x, "fs", [(i, i ^ mask) for i in range(lax.axis_size("fs"))])


def tp_xor(x, mask):
    return lax.ppermute(x, "tp", [(i, i ^ mask) for i in range(lax.axis_size("tp"))])


def scale_rows(x):
    level = jnp.log2(jnp.maximum(jnp.max(jnp.abs(x)), 1e-30))
    high = level.astype(jnp.float16)
    low = (level - high.astype(jnp.float32)).astype(jnp.float16)
    return high, low


def encode(x, high, low):
    factor = 16384.0 * jnp.exp2(-(high.astype(jnp.float32) + low.astype(jnp.float32)))
    body = (x * factor).astype(jnp.float16)
    rows = lax.broadcasted_iota(jnp.int32, (8, x.shape[1]), 0)
    return jnp.concatenate([body, jnp.where(rows == 0, high, low)], axis=0)


def decode(y):
    level = y[-8, 0].astype(jnp.float32) + y[-7, 0].astype(jnp.float32)
    return y[:-8].astype(jnp.float32) * (jnp.exp2(level) / 16384.0)


def finish(place, in_direction, point_direction, in_basis, point_basis, masters, blocks):
    rows, cols = masters[0].shape
    full = in_basis.shape[0]
    count = len(blocks)

    def kernel(place_ref, din, dpt, bin_, bpt, min_, mpt, *rest):
        block_refs = rest[: count * CORES]
        outs = rest[count * CORES : count * CORES + 6]
        stage, own, sems = rest[count * CORES + 6 :]
        z = place_ref[0]
        me = place_ref[1]
        copies = []
        halves = []
        for d in (din, dpt):
            value = d[...]
            high = value.astype(jnp.bfloat16)
            low = (value - high.astype(jnp.float32)).astype(jnp.bfloat16)
            halves.append(jnp.concatenate([high, low], axis=0))

        def product(which, row0):
            b = (bin_, bpt)[which][pl.ds(row0, rows), :]
            both = jnp.concatenate([b, b], axis=1)
            return -jnp.dot(both, halves[which], preferred_element_type=jnp.float32)

        n = 0
        for which in range(2):
            step = product(which, me * rows)
            own[which] = step
            own[2 + which] = (min_, mpt)[which][...] + step
            for j in (which, 2 + which):
                copies.append(pltpu.make_async_copy(own.at[j], outs[j], sems.at[n]))
                copies[-1].start()
                n += 1
        for k in range(count):
            for c in range(CORES):
                row0 = (CORES * (z ^ k) + c) * rows
                for which in range(2):
                    old = block_refs[k * CORES + c][which * rows : (which + 1) * rows, :]
                    slot = (k * CORES + c) * 2 + which
                    stage[slot] = (old + product(which, row0)).astype(jnp.bfloat16)
                    copies.append(
                        pltpu.make_async_copy(
                            stage.at[slot], outs[4 + which].at[pl.ds(row0, rows), :], sems.at[n]
                        )
                    )
                    copies[-1].start()
                    n += 1
        for copy in copies:
            copy.wait()

    vmem = pl.BlockSpec(memory_space=pltpu.VMEM)
    hbm = pl.BlockSpec(memory_space=pl.ANY)
    n_copies = 4 + count * CORES * 2
    flat = [b for pair in blocks for b in pair]
    return pl.pallas_call(
        kernel,
        out_shape=[jax.ShapeDtypeStruct((rows, cols), jnp.float32)] * 4
        + [jax.ShapeDtypeStruct((full, cols), jnp.bfloat16)] * 2,
        in_specs=[pl.BlockSpec(memory_space=pltpu.SMEM)] + [vmem] * (6 + len(flat)),
        out_specs=[hbm] * 6,
        scratch_shapes=[
            pltpu.VMEM((count * CORES * 2, rows, cols), jnp.bfloat16),
            pltpu.VMEM((4, rows, cols), jnp.float32),
            pltpu.SemaphoreType.DMA((n_copies,)),
        ],
        name="finish",
    )(place, in_direction, point_direction, in_basis, point_basis, *masters, *flat)


def short_body(
    in_saved,
    in_cotangent,
    point_saved,
    point_cotangent,
    in_basis,
    point_basis,
    in_first,
    in_second,
    point_first,
    point_second,
    in_master,
    point_master,
):
    fs_count = lax.axis_size("fs")
    tp_count = lax.axis_size("tp")
    z_count = fs_count // CORES
    me = lax.axis_index("fs")
    column = lax.axis_index("tp")
    z = me // CORES
    core = me % CORES
    rows, cols = in_master.shape
    rank_here = in_first.shape[0]

    own = jnp.concatenate(
        [in_master, point_master, in_first, in_second, point_first, point_second], axis=0
    ).astype(jnp.float16)
    one = fs_xor(own, CORES)
    three = fs_xor(own, 3 * CORES)

    in_low = low_term(in_saved, in_cotangent, in_basis)
    point_low = low_term(point_saved, point_cotangent, point_basis)
    rank = in_low.shape[0]
    entries = 1.0 * rank * (in_low.shape[1] + point_low.shape[1])
    first_core = core == 0
    given = fs_xor(jnp.where(first_core, point_low, in_low), 1)
    chip = jnp.where(first_core, in_low, point_low) + given

    high, low = scale_rows(chip)
    coded = encode(chip, high, low)
    plane = lax.dynamic_slice_in_dim(chip, column * cols, cols, 1)
    got = [
        tp_xor(lax.dynamic_slice_in_dim(coded, (column ^ k) * cols, cols, 1), k)
        for k in range(1, tp_count)
    ]
    for g in got:
        plane = plane + decode(g)

    two = fs_xor(three, CORES)

    high, low = scale_rows(plane)
    coded = encode(plane, high, low)
    got = [fs_xor(coded, CORES * k) for k in range(1, z_count)]
    total = plane
    for g in got:
        total = total + decode(g)
    other = fs_xor(total, 1)
    sum_in = jnp.where(first_core, total, other)
    sum_point = jnp.where(first_core, other, total)
    squares = jnp.sum(total * total) + jnp.sum(other * other)
    squares = jnp.full((8, 128), squares, jnp.float32)
    got = [tp_xor(squares, k) for k in range(1, tp_count)]
    for g in got:
        squares = squares + g
    clip_factor = clip_of(squares[0, 0], entries)
    grad_in = clip_factor * sum_in
    grad_point = clip_factor * sum_point

    mine = [own, one, two, three]
    theirs = [fs_xor(b, 1) for b in mine]
    pairs = [
        [jnp.where(first_core, a, b), jnp.where(first_core, b, a)]
        for a, b in zip(mine, theirs)
    ]
    olds = [[p[: 2 * rows].astype(jnp.float32) for p in pair] for pair in pairs]
    old_moments = []
    for j in range(4):
        lo = 2 * rows + j * rank_here
        stack = jnp.concatenate([p[lo : lo + rank_here] for pair in pairs for p in pair], axis=0)
        stack = stack.astype(jnp.float32).reshape(z_count, CORES * rank_here, cols)
        order = jnp.arange(z_count) ^ z
        old_moments.append(jnp.take(stack, order, axis=0).reshape(rank, cols))
    in_direction = moments(old_moments[0], old_moments[1], grad_in)[2]
    point_direction = moments(old_moments[2], old_moments[3], grad_point)[2]

    def here(a):
        return lax.dynamic_slice_in_dim(a, me * rank_here, rank_here, 0)

    in_first_new, in_second_new, _ = moments(in_first, in_second, here(grad_in))
    point_first_new, point_second_new, _ = moments(point_first, point_second, here(grad_point))
    place = jnp.stack([z, me]).astype(jnp.int32)
    finished = finish(
        place,
        in_direction,
        point_direction,
        in_basis,
        point_basis,
        (in_master, point_master),
        olds,
    )
    return (in_first_new, in_second_new, point_first_new, point_second_new, *finished)


def solution(mesh):
    z_count = mesh.shape["fs"] // CORES
    tp_count = mesh.shape["tp"]
    short = z_count == 4 and tp_count == 4
    return jax.shard_map(
        short_body if short else plain_body,
        mesh=mesh,
        in_specs=(P(("fs", "tp"), None),) * 4 + (P(),) * 2 + (P("fs", "tp"),) * 6,
        out_specs=(P("fs", "tp"),) * 8 + (P(None, "tp"),) * 2,
        check_vma=False,
    )
```

```python
import jax
import jax.numpy as jnp
from jax import lax
from jax.experimental import pallas as pl
from jax.experimental.pallas import tpu as pltpu
from jax.sharding import PartitionSpec as P


CORES = 2


def low_term(saved, cotangent, basis):
    reduced = jnp.dot(saved, basis, preferred_element_type=jnp.float32).astype(jnp.bfloat16)
    return lax.dot_general(
        reduced, cotangent, (((0,), (0,)), ((), ())), preferred_element_type=jnp.float32
    )


def moments(first, second, grad):
    first_new = 0.8 * first + 0.2 * grad
    second_new = 0.9 * second + 0.1 * grad * grad
    return (first_new, second_new, first_new / (jnp.sqrt(second_new) + 1e-08))


def weight_step(basis, direction, fs_count):
    row_count = basis.shape[0] // fs_count
    rows_here = lax.dynamic_slice_in_dim(basis, lax.axis_index("fs") * row_count, row_count, 0)
    return -jnp.dot(rows_here.astype(jnp.float32), direction, precision=lax.Precision.HIGHEST)


def clip_of(squares, entries):
    return jnp.minimum(1.0, 1.0 / jnp.sqrt(squares / entries + 1e-06))


def plain_body(
    in_saved,
    in_cotangent,
    point_saved,
    point_cotangent,
    in_basis,
    point_basis,
    in_first,
    in_second,
    point_first,
    point_second,
    in_master,
    point_master,
):
    fs_count = lax.axis_size("fs")
    in_low = low_term(in_saved, in_cotangent, in_basis)
    point_low = low_term(point_saved, point_cotangent, point_basis)
    rank_rows = in_low.shape[0]
    entries = 1.0 * rank_rows * (in_low.shape[1] + point_low.shape[1])
    part_in, part_point = (
        lax.psum_scatter(in_low, "tp", scatter_dimension=1, tiled=True),
        lax.psum_scatter(point_low, "tp", scatter_dimension=1, tiled=True),
    )
    sum_in, sum_point = lax.psum((part_in, part_point), "fs")
    squares = lax.psum(jnp.sum(sum_in * sum_in) + jnp.sum(sum_point * sum_point), "tp")
    clip_factor = clip_of(squares, entries)
    previous = tuple(
        lax.all_gather(a, "fs", axis=0, tiled=True)
        for a in (in_first, in_second, point_first, point_second)
    )
    in_first_all, in_second_all, in_direction = moments(
        previous[0], previous[1], clip_factor * sum_in
    )
    point_first_all, point_second_all, point_direction = moments(
        previous[2], previous[3], clip_factor * sum_point
    )
    row_count = rank_rows // fs_count
    row_start = lax.axis_index("fs") * row_count
    mine = tuple(
        lax.dynamic_slice_in_dim(a, row_start, row_count, 0)
        for a in (in_first_all, in_second_all, point_first_all, point_second_all)
    )
    in_step = weight_step(in_basis, in_direction, fs_count)
    point_step = weight_step(point_basis, point_direction, fs_count)
    in_master_new = in_master + in_step
    point_master_new = point_master + point_step
    in_copy, point_copy = (
        lax.all_gather(in_master_new.astype(jnp.bfloat16), "fs", axis=0, tiled=True),
        lax.all_gather(point_master_new.astype(jnp.bfloat16), "fs", axis=0, tiled=True),
    )
    return (*mine, in_step, point_step, in_master_new, point_master_new, in_copy, point_copy)


def exchange(x, fs_mask, tp_mask=0):
    fs_count, tp_count = lax.axis_size("fs"), lax.axis_size("tp")
    pairs = [
        (f * tp_count + t, (f ^ fs_mask) * tp_count + (t ^ tp_mask))
        for f in range(fs_count)
        for t in range(tp_count)
    ]
    return lax.ppermute(x, ("fs", "tp"), pairs)


PLAIN_UNIT = 2.0**-14
VMEM = pl.BlockSpec(memory_space=pltpu.VMEM)
HBM = pl.BlockSpec(memory_space=pltpu.HBM)
TAG = 8


def shape(*dims, dtype=jnp.float32):
    return jax.ShapeDtypeStruct(dims, dtype)


def code(y):
    y2 = y * y
    y4 = y2 * y2
    y8 = y4 * y4
    return jnp.where(y < 0.0, -y8, y8).astype(jnp.bfloat16)


def uncode(t):
    t = t.astype(jnp.float32)
    size = jnp.exp2(jnp.log2(jnp.abs(t)) * 0.125)
    return jnp.where(t < 0.0, -size, size)


def unit_for(largest):
    unit = jnp.maximum(largest, 1e-30) * (1.0156 * 2.0**-15.75)
    return unit.astype(jnp.bfloat16)


def call(kernel, outs, args, mib, hbm_args=False, hbm_outs=False, scratch=()):
    return pl.pallas_call(
        kernel,
        out_shape=outs,
        in_specs=[HBM if hbm_args else VMEM] * len(args),
        out_specs=[HBM if hbm_outs else VMEM] * len(outs),
        scratch_shapes=scratch,
        compiler_params=pltpu.CompilerParams(vmem_limit_bytes=mib << 20),
    )(*args)


def begin(stored, saved, cotangents, bases):
    rank, width = bases[0].shape[1], cotangents[0].shape[1]
    cols = stored[0][0].shape[1]
    packed = sum(a.shape[0] for a in stored[0])
    first = len(stored[0])
    arrays = (*stored[0], *stored[1], bases[0], saved[0], cotangents[0], bases[1], saved[1], cotangents[1])
    count = len(arrays)

    def kernel(*refs):
        sources, outs = refs[:count], refs[count : count + 4]
        held, sems = refs[count + 4 : 2 * count + 4], refs[2 * count + 4]
        core = lax.axis_index("fs") % CORES
        copies = [
            pltpu.make_async_copy(src, dst, sems.at[n])
            for n, (src, dst) in enumerate(zip(sources, held))
        ]
        for copy in copies:
            copy.start()
        for which in range(2):
            row = 0
            for n in range(which * first, (which + 1) * first):
                copies[n].wait()
                size = held[n].shape[0]
                outs[which][row : row + size, :] = code(held[n][...] * (1.0 / PLAIN_UNIT))
                row += size
        for which in range(2):
            at = 2 * first + 3 * which
            copies[at].wait()
            copies[at + 1].wait()
            reduced = jnp.dot(
                held[at + 1][...], held[at][...], preferred_element_type=jnp.float32
            )
            copies[at + 2].wait()
            term = lax.dot_general(
                reduced.astype(jnp.bfloat16),
                held[at + 2][...],
                (((0,), (0,)), ((), ())),
                preferred_element_type=jnp.float32,
            )

            @pl.when(core == which)
            def _():
                outs[3][...] = term

            @pl.when(core != which)
            def _():
                outs[2][...] = term

    scratch = [pltpu.VMEM(a.shape, a.dtype) for a in arrays] + [pltpu.SemaphoreType.DMA((count,))]
    outs = [shape(packed, cols, dtype=jnp.bfloat16)] * 2 + [shape(rank, width)] * 2
    return call(kernel, outs, arrays, 60, hbm_args=True, scratch=scratch)


def put_coded(ref, value, unit):
    rank = value.shape[0]
    ref[:rank, :] = code(value * (1.0 / unit.astype(jnp.float32)))
    ref[rank:, :] = jnp.full((TAG, ref.shape[1]), unit, jnp.bfloat16)


def get_coded(ref):
    rank = ref.shape[0] - TAG
    return uncode(ref[:rank, :]) * ref[rank:, :].astype(jnp.float32)[:1, :1]


def chip_sum(keep, given, count):
    rank, width = keep.shape
    cols = width // count

    def kernel(keep, given, mine, *rest):
        coded, total = rest[:-1], rest[-1]
        column = lax.axis_index("tp")
        value = keep[...] + given[...]
        total[...] = value
        unit = unit_for(jnp.max(jnp.abs(value)))
        mine[...] = total[:, pl.ds(pl.multiple_of(column * cols, cols), cols)]
        for k in range(1, count):
            at = pl.multiple_of((column ^ k) * cols, cols)
            put_coded(coded[k - 1], total[:, pl.ds(at, cols)], unit)

    outs = [shape(rank, cols)] + [shape(rank + TAG, cols, dtype=jnp.bfloat16)] * (count - 1)
    scratch = [pltpu.VMEM((rank, width), jnp.float32)]
    return call(kernel, outs, (keep, given), 8, scratch=scratch)


def plane_sum(mine, got):
    def kernel(mine, *refs):
        value = mine[...]
        for ref in refs[:-1]:
            value = value + get_coded(ref)
        put_coded(refs[-1], value, unit_for(jnp.max(jnp.abs(value))))

    outs = [shape(mine.shape[0] + TAG, mine.shape[1], dtype=jnp.bfloat16)]
    return call(kernel, outs, (mine, *got), 8)[0]


def pair_sum(a, b, last):
    def kernel(a, b, out):
        value = get_coded(a) + get_coded(b)
        if last:
            out[...] = value
        else:
            put_coded(out, value, unit_for(jnp.max(jnp.abs(value))))

    rows, cols = a.shape
    out = shape(rows - TAG, cols) if last else shape(rows, cols, dtype=a.dtype)
    return call(kernel, [out], (a, b), 8)[0]


def square_sum(a, b):
    def kernel(a, b, out):
        value = jnp.sum(a[...] * a[...]) + jnp.sum(b[...] * b[...])
        out[...] = jnp.full(out.shape, value, jnp.float32)

    return call(kernel, [shape(8, 128)], (a, b), 4)[0]


def finish(entries, total, other, squares, bases, masters, old, blocks):
    rows, cols = masters[0].shape
    full, rank = bases[0].shape
    here = old[0].shape[0]
    n_sq, n_bl = len(squares), len(blocks)

    def kernel(*refs):
        refs = list(refs)

        def take(n):
            part = refs[:n]
            del refs[:n]
            return part

        total, other = take(2)
        square_refs = take(n_sq)
        basis_refs = take(2)
        master_refs = take(2)
        old_refs = take(4)
        block_refs = [take(2) for _ in range(n_bl)]
        outs = take(10)
        grads, direction, small, own, stage, sems = refs
        me = lax.axis_index("fs")
        core = me % CORES
        copies = []

        def send(src, dst):
            copies.append(pltpu.make_async_copy(src, dst, sems.at[len(copies)]))
            copies[-1].start()

        squares = square_refs[0][...]
        for ref in square_refs[1:]:
            squares = squares + ref[...]
        clip = clip_of(squares[:1, :1], entries)
        mine = total[...] * clip
        theirs = other[...] * clip
        grads[0] = jnp.where(core == 0, mine, theirs)
        grads[1] = jnp.where(core == 0, theirs, mine)
        for which in range(2):
            grad = grads[which, pl.ds(pl.multiple_of(me * here, here), here), :]
            new = moments(old_refs[2 * which][...], old_refs[2 * which + 1][...], grad)
            for j in range(2):
                small[2 * which + j] = new[j]
                send(small.at[2 * which + j], outs[2 * which + j])
        for n in range(n_bl):
            at = pl.multiple_of((me ^ n) * here, here)
            for which in range(2):
                ref = block_refs[n][which]
                first = uncode(ref[rows : rows + here, :]) * PLAIN_UNIT
                second = uncode(ref[rows + here : rows + 2 * here, :]) * PLAIN_UNIT
                value = moments(first, second, grads[which, pl.ds(at, here), :])[2]
                high = value.astype(jnp.bfloat16)
                direction[which, pl.ds(at, here), :] = high
                direction[which, pl.ds(pl.multiple_of(rank + at, here), here), :] = (
                    value - high.astype(jnp.float32)
                ).astype(jnp.bfloat16)

        for n in range(n_bl):
            row0 = pl.multiple_of((me ^ n) * rows, rows)
            for which in range(2):
                b = basis_refs[which][pl.ds(row0, rows), :]
                both = jnp.concatenate([b, b], axis=1)
                down = jnp.dot(both, direction[which], preferred_element_type=jnp.float32)
                if n == 0:
                    own[which] = -down
                    own[2 + which] = master_refs[which][...] - down
                    for j in (which, 2 + which):
                        send(own.at[j], outs[4 + j])
                value = uncode(block_refs[n][which][:rows, :]) * PLAIN_UNIT
                stage[2 * n + which] = (value - down).astype(jnp.bfloat16)
                send(stage.at[2 * n + which], outs[8 + which].at[pl.ds(row0, rows), :])
        for copy in copies:
            copy.wait()

    outs = [shape(here, cols)] * 4 + [shape(rows, cols)] * 4
    outs += [shape(full, cols, dtype=jnp.bfloat16)] * 2
    flat = [array for block in blocks for array in block]
    args = (total, other, *squares, *bases, *masters, *old, *flat)
    scratch = [
        pltpu.VMEM((2, rank, cols), jnp.float32),
        pltpu.VMEM((2, 2 * rank, cols), jnp.bfloat16),
        pltpu.VMEM((4, here, cols), jnp.float32),
        pltpu.VMEM((4, rows, cols), jnp.float32),
        pltpu.VMEM((2 * n_bl, rows, cols), jnp.bfloat16),
        pltpu.SemaphoreType.DMA((8 + 2 * n_bl,)),
    ]
    return call(kernel, outs, args, 24, hbm_outs=True, scratch=scratch)


def short_body(
    in_saved,
    in_cotangent,
    point_saved,
    point_cotangent,
    in_basis,
    point_basis,
    in_first,
    in_second,
    point_first,
    point_second,
    in_master,
    point_master,
):
    tp_count = lax.axis_size("tp")
    rank = in_basis.shape[1]
    entries = 1.0 * rank * (in_cotangent.shape[1] + point_cotangent.shape[1])
    masters = (in_master, point_master)
    old = (in_first, in_second, point_first, point_second)
    bases = (in_basis, point_basis)

    *packs, give, keep = begin(
        ((in_master, in_first, in_second), (point_master, point_first, point_second)),
        (in_saved, point_saved),
        (in_cotangent, point_cotangent),
        bases,
    )
    given = exchange(give, 1)
    one = [exchange(p, CORES) for p in packs]
    three = [exchange(p, 3 * CORES) for p in packs]

    mine, *coded = chip_sum(keep, given, tp_count)
    got = [exchange(coded[k - 1], 0, k) for k in range(1, tp_count)]
    coded = plane_sum(mine, got)
    coded = pair_sum(coded, exchange(coded, CORES), False)
    total = pair_sum(coded, exchange(coded, 2 * CORES), True)
    two = [exchange(t, CORES) for t in three]
    other = exchange(total, 1)
    squares = square_sum(total, other)
    squares = [squares] + [exchange(squares, 0, k) for k in range(1, tp_count)]
    blocks = []
    for arrays in (packs, one, two, three):
        swapped = [exchange(a, 1) for a in arrays]
        blocks += [arrays, swapped]
    return tuple(finish(entries, total, other, squares, bases, masters, old, blocks))


def solution(mesh):
    z_count = mesh.shape["fs"] // CORES
    tp_count = mesh.shape["tp"]
    short = z_count == 4 and tp_count == 4
    return jax.shard_map(
        short_body if short else plain_body,
        mesh=mesh,
        in_specs=(P(("fs", "tp"), None),) * 4 + (P(),) * 2 + (P("fs", "tp"),) * 6,
        out_specs=(P("fs", "tp"),) * 8 + (P(None, "tp"),) * 2,
        check_vma=False,
    )
```

```python
import jax
import jax.numpy as jnp
from jax import lax
from jax.experimental import pallas as pl
from jax.experimental.pallas import tpu as pltpu
from jax.sharding import PartitionSpec as P


CORES = 2


def low_term(saved, cotangent, basis):
    reduced = jnp.dot(saved, basis, preferred_element_type=jnp.float32).astype(jnp.bfloat16)
    return lax.dot_general(
        reduced, cotangent, (((0,), (0,)), ((), ())), preferred_element_type=jnp.float32
    )


def moments(first, second, grad):
    first_new = 0.8 * first + 0.2 * grad
    second_new = 0.9 * second + 0.1 * grad * grad
    return (first_new, second_new, first_new / (jnp.sqrt(second_new) + 1e-08))


def weight_step(basis, direction, fs_count):
    row_count = basis.shape[0] // fs_count
    rows_here = lax.dynamic_slice_in_dim(basis, lax.axis_index("fs") * row_count, row_count, 0)
    return -jnp.dot(rows_here.astype(jnp.float32), direction, precision=lax.Precision.HIGHEST)


def clip_of(squares, entries):
    return jnp.minimum(1.0, 1.0 / jnp.sqrt(squares / entries + 1e-06))


def plain_body(
    in_saved,
    in_cotangent,
    point_saved,
    point_cotangent,
    in_basis,
    point_basis,
    in_first,
    in_second,
    point_first,
    point_second,
    in_master,
    point_master,
):
    fs_count = lax.axis_size("fs")
    in_low = low_term(in_saved, in_cotangent, in_basis)
    point_low = low_term(point_saved, point_cotangent, point_basis)
    rank_rows = in_low.shape[0]
    entries = 1.0 * rank_rows * (in_low.shape[1] + point_low.shape[1])
    part_in, part_point = (
        lax.psum_scatter(in_low, "tp", scatter_dimension=1, tiled=True),
        lax.psum_scatter(point_low, "tp", scatter_dimension=1, tiled=True),
    )
    sum_in, sum_point = lax.psum((part_in, part_point), "fs")
    squares = lax.psum(jnp.sum(sum_in * sum_in) + jnp.sum(sum_point * sum_point), "tp")
    clip_factor = clip_of(squares, entries)
    previous = tuple(
        lax.all_gather(a, "fs", axis=0, tiled=True)
        for a in (in_first, in_second, point_first, point_second)
    )
    in_first_all, in_second_all, in_direction = moments(
        previous[0], previous[1], clip_factor * sum_in
    )
    point_first_all, point_second_all, point_direction = moments(
        previous[2], previous[3], clip_factor * sum_point
    )
    row_count = rank_rows // fs_count
    row_start = lax.axis_index("fs") * row_count
    mine = tuple(
        lax.dynamic_slice_in_dim(a, row_start, row_count, 0)
        for a in (in_first_all, in_second_all, point_first_all, point_second_all)
    )
    in_step = weight_step(in_basis, in_direction, fs_count)
    point_step = weight_step(point_basis, point_direction, fs_count)
    in_master_new = in_master + in_step
    point_master_new = point_master + point_step
    in_copy, point_copy = (
        lax.all_gather(in_master_new.astype(jnp.bfloat16), "fs", axis=0, tiled=True),
        lax.all_gather(point_master_new.astype(jnp.bfloat16), "fs", axis=0, tiled=True),
    )
    return (*mine, in_step, point_step, in_master_new, point_master_new, in_copy, point_copy)


def exchange(x, fs_mask, tp_mask=0):
    fs_count, tp_count = lax.axis_size("fs"), lax.axis_size("tp")
    pairs = [
        (f * tp_count + t, (f ^ fs_mask) * tp_count + (t ^ tp_mask))
        for f in range(fs_count)
        for t in range(tp_count)
    ]
    return lax.ppermute(x, ("fs", "tp"), pairs)


PLAIN_UNIT = 2.0**-14
VMEM = pl.BlockSpec(memory_space=pltpu.VMEM)
HBM = pl.BlockSpec(memory_space=pltpu.HBM)
TAG = 8
PIECES = 2
CUTS = (3,)


def shape(*dims, dtype=jnp.float32):
    return jax.ShapeDtypeStruct(dims, dtype)


def code(y):
    y2 = y * y
    y4 = y2 * y2
    y8 = y4 * y4
    return jnp.where(y < 0.0, -y8, y8).astype(jnp.bfloat16)


def uncode(t):
    t = t.astype(jnp.float32)
    size = jnp.exp2(jnp.log2(jnp.abs(t)) * 0.125)
    return jnp.where(t < 0.0, -size, size)


def unit_for(largest):
    unit = jnp.maximum(largest, 1e-30) * (1.0156 * 2.0**-15.75)
    return unit.astype(jnp.bfloat16)


def call(kernel, outs, args, mib, hbm_args=False, hbm_outs=False, scratch=()):
    return pl.pallas_call(
        kernel,
        out_shape=outs,
        in_specs=[HBM if hbm_args else VMEM] * len(args),
        out_specs=[HBM if hbm_outs else VMEM] * len(outs),
        scratch_shapes=scratch,
        compiler_params=pltpu.CompilerParams(vmem_limit_bytes=mib << 20),
    )(*args)


def in_hbm(arrays):
    return [pltpu.with_memory_space_constraint(a, pltpu.HBM) for a in arrays]


def pack(stored, cuts):
    cols = stored[0].shape[1]
    packed = sum(a.shape[0] for a in stored)
    count = len(stored)
    edges = [0, *cuts, packed]

    def kernel(*refs):
        sources, outs = refs[:count], refs[count : count + len(edges)]
        held, sems = refs[count + len(edges) : -1], refs[-1]
        copies = [
            pltpu.make_async_copy(src, dst, sems.at[n])
            for n, (src, dst) in enumerate(zip(sources, held))
        ]
        for copy in copies:
            copy.start()
        row = 0
        for n in range(count):
            copies[n].wait()
            size = held[n].shape[0]
            value = code(held[n][...] * (1.0 / PLAIN_UNIT))
            outs[0][row : row + size, :] = value
            for part, low, high in zip(outs[1:], edges, edges[1:]):
                first, last = max(low, row), min(high, row + size)
                if first < last:
                    part[first - low : last - low, :] = value[first - row : last - row, :]
            row += size

    scratch = [pltpu.VMEM(a.shape, a.dtype) for a in stored]
    scratch += [pltpu.SemaphoreType.DMA((count,))]
    sizes = [packed] + [high - low for low, high in zip(edges, edges[1:])]
    outs = [shape(n, cols, dtype=jnp.bfloat16) for n in sizes]
    return call(kernel, outs, in_hbm(stored), 6, hbm_args=True, scratch=scratch)


def low_terms(saved, cotangents, bases):
    rank, width = bases[0].shape[1], cotangents[0].shape[1]
    arrays = (bases[0], saved[0], bases[1], saved[1], *cotangents)
    count = len(arrays)

    def kernel(*refs):
        sources, (give, keep) = refs[:count], refs[count : count + 2]
        held, sems = refs[count + 2 : 2 * count + 2], refs[2 * count + 2]
        core = lax.axis_index("fs") % CORES
        copies = [
            pltpu.make_async_copy(src, dst, sems.at[n])
            for n, (src, dst) in enumerate(zip(sources, held))
        ]
        for copy in copies:
            copy.start()
        reduced = []
        for which in range(2):
            copies[2 * which].wait()
            copies[2 * which + 1].wait()
            value = jnp.dot(
                held[2 * which + 1][...], held[2 * which][...], preferred_element_type=jnp.float32
            )
            reduced.append(value.astype(jnp.bfloat16))
        for which in range(2):
            copies[4 + which].wait()
            term = lax.dot_general(
                reduced[which],
                held[4 + which][...],
                (((0,), (0,)), ((), ())),
                preferred_element_type=jnp.float32,
            )

            @pl.when(core == which)
            def _():
                keep[...] = term

            @pl.when(core != which)
            def _():
                give[...] = term

    scratch = [pltpu.VMEM(a.shape, a.dtype) for a in arrays]
    scratch += [pltpu.SemaphoreType.DMA((count,))]
    outs = [shape(rank, width)] * 2
    return call(kernel, outs, in_hbm(arrays), 12, hbm_args=True, scratch=scratch)


def put_coded(ref, value, unit):
    rank = value.shape[0]
    ref[:rank, :] = code(value * (1.0 / unit.astype(jnp.float32)))
    ref[rank:, :] = jnp.full((TAG, ref.shape[1]), unit, jnp.bfloat16)


def get_coded(ref):
    rank = ref.shape[0] - TAG
    return uncode(ref[:rank, :]) * ref[rank:, :].astype(jnp.float32)[:1, :1]


def chip_sum(keep, given, count):
    rank, width = keep.shape
    cols = width // count

    def kernel(keep, given, mine, *rest):
        coded, total = rest[:-1], rest[-1]
        column = lax.axis_index("tp")
        value = keep[...] + given[...]
        total[...] = value
        unit = unit_for(jnp.max(jnp.abs(value)))
        mine[...] = total[:, pl.ds(pl.multiple_of(column * cols, cols), cols)]
        for k in range(1, count):
            at = pl.multiple_of((column ^ k) * cols, cols)
            put_coded(coded[k - 1], total[:, pl.ds(at, cols)], unit)

    outs = [shape(rank, cols)] + [shape(rank + TAG, cols, dtype=jnp.bfloat16)] * (count - 1)
    scratch = [pltpu.VMEM((rank, width), jnp.float32)]
    return call(kernel, outs, (keep, given), 8, scratch=scratch)


def plane_sum(mine, got):
    def kernel(mine, *refs):
        value = mine[...]
        for ref in refs[:-1]:
            value = value + get_coded(ref)
        put_coded(refs[-1], value, unit_for(jnp.max(jnp.abs(value))))

    outs = [shape(mine.shape[0] + TAG, mine.shape[1], dtype=jnp.bfloat16)]
    return call(kernel, outs, (mine, *got), 8)[0]


def pair_sum(a, b, last):
    def kernel(a, b, out):
        value = get_coded(a) + get_coded(b)
        if last:
            out[...] = value
        else:
            put_coded(out, value, unit_for(jnp.max(jnp.abs(value))))

    rows, cols = a.shape
    out = shape(rows - TAG, cols) if last else shape(rows, cols, dtype=a.dtype)
    return call(kernel, [out], (a, b), 8)[0]


def square_sum(a, b):
    def kernel(a, b, out):
        value = jnp.sum(a[...] * a[...]) + jnp.sum(b[...] * b[...])
        out[...] = jnp.full(out.shape, value, jnp.float32)

    return call(kernel, [shape(8, 128)], (a, b), 4)[0]


def finish(entries, total, other, squares, bases, masters, old, blocks):
    rows, cols = masters[0].shape
    full, rank = bases[0].shape
    here = old[0].shape[0]
    n_sq, n_bl = len(squares), len(blocks)
    piece = rows // PIECES
    flat = [a for block in blocks for a in block]

    def kernel(*refs):
        refs = list(refs)

        def take(n):
            part = refs[:n]
            del refs[:n]
            return part

        total, other = take(2)
        square_refs = take(n_sq)
        basis_refs = take(2)
        master_refs = take(2)
        old_refs = take(4)
        block_refs = [take(len(block)) for block in blocks]
        outs = take(10)
        grads, direction, small, own, stage, sems = refs
        me = lax.axis_index("fs")
        core = me % CORES
        copies = []

        def send(src, dst):
            copies.append(pltpu.make_async_copy(src, dst, sems.at[len(copies)]))
            copies[-1].start()

        def packed(n, row, size):
            for ref in block_refs[n]:
                if row < ref.shape[0]:
                    return uncode(ref[row : row + size, :]) * PLAIN_UNIT
                row -= ref.shape[0]

        squares = square_refs[0][...]
        for ref in square_refs[1:]:
            squares = squares + ref[...]
        clip = clip_of(squares[:1, :1], entries)
        mine = total[...] * clip
        theirs = other[...] * clip
        grads[0] = jnp.where(core == 0, mine, theirs)
        grads[1] = jnp.where(core == 0, theirs, mine)
        for which in range(2):
            for n in range(n_bl):
                at = pl.multiple_of((me ^ n) * here, here)
                first = packed(n, 2 * which * here, here)
                second = packed(n, (2 * which + 1) * here, here)
                value = moments(first, second, grads[which, pl.ds(at, here), :])[2]
                high = value.astype(jnp.bfloat16)
                direction[which, pl.ds(at, here), :] = high
                direction[which, pl.ds(pl.multiple_of(rank + at, here), here), :] = (
                    value - high.astype(jnp.float32)
                ).astype(jnp.bfloat16)
            for n in range(n_bl):
                for p in range(PIECES):
                    row0 = pl.multiple_of((me ^ n) * rows + p * piece, piece)
                    b = basis_refs[which][pl.ds(row0, piece), :]
                    both = jnp.concatenate([b, b], axis=1)
                    down = jnp.dot(both, direction[which], preferred_element_type=jnp.float32)
                    at = slice(p * piece, (p + 1) * piece)
                    if n == 0:
                        own[which, at, :] = -down
                        own[2 + which, at, :] = master_refs[which][at, :] - down
                    value = packed(n, 4 * here + which * rows + p * piece, piece)
                    stage[2 * n + which, at, :] = (value - down).astype(jnp.bfloat16)
                if n == 0:
                    for j in (which, 2 + which):
                        send(own.at[j], outs[4 + j])
                row0 = pl.multiple_of((me ^ n) * rows, rows)
                send(stage.at[2 * n + which], outs[8 + which].at[pl.ds(row0, rows), :])
        for which in range(2):
            grad = grads[which, pl.ds(pl.multiple_of(me * here, here), here), :]
            new = moments(old_refs[2 * which][...], old_refs[2 * which + 1][...], grad)
            for j in range(2):
                small[2 * which + j] = new[j]
                send(small.at[2 * which + j], outs[2 * which + j])
        for copy in copies:
            copy.wait()

    outs = [shape(here, cols)] * 4 + [shape(rows, cols)] * 4
    outs += [shape(full, cols, dtype=jnp.bfloat16)] * 2
    args = (total, other, *squares, *bases, *masters, *old, *flat)
    scratch = [
        pltpu.VMEM((2, rank, cols), jnp.float32),
        pltpu.VMEM((2, 2 * rank, cols), jnp.bfloat16),
        pltpu.VMEM((4, here, cols), jnp.float32),
        pltpu.VMEM((4, rows, cols), jnp.float32),
        pltpu.VMEM((2 * n_bl, rows, cols), jnp.bfloat16),
        pltpu.SemaphoreType.DMA((8 + 2 * n_bl,)),
    ]
    return call(kernel, outs, args, 24, hbm_outs=True, scratch=scratch)


def short_body(
    in_saved,
    in_cotangent,
    point_saved,
    point_cotangent,
    in_basis,
    point_basis,
    in_first,
    in_second,
    point_first,
    point_second,
    in_master,
    point_master,
):
    tp_count = lax.axis_size("tp")
    rank = in_basis.shape[1]
    entries = 1.0 * rank * (in_cotangent.shape[1] + point_cotangent.shape[1])
    masters = (in_master, point_master)
    old = (in_first, in_second, point_first, point_second)
    bases = (in_basis, point_basis)

    piece = in_master.shape[0] // PIECES
    at = [len(old) * in_first.shape[0] + n * piece for n in CUTS]
    whole, *parts = pack((*old, *masters), at)
    one = exchange(whole, CORES)
    three = [exchange(p, 3 * CORES) for p in parts]

    give, keep = low_terms(
        (in_saved, point_saved), (in_cotangent, point_cotangent), bases
    )
    given = exchange(give, 1)
    mine, *coded = chip_sum(keep, given, tp_count)
    got = [exchange(coded[k - 1], 0, k) for k in range(1, tp_count)]
    coded = plane_sum(mine, got)
    coded = pair_sum(coded, exchange(coded, CORES), False)
    total = pair_sum(coded, exchange(coded, 2 * CORES), True)
    two = [exchange(t, CORES) for t in three]

    other = exchange(total, 1)
    squares = square_sum(total, other)
    squares = [squares] + [exchange(squares, 0, k) for k in range(1, tp_count)]

    blocks = [[whole], [exchange(whole, 1)], [one], [exchange(one, 1)]]
    for arrays in (two, three):
        blocks += [arrays, [exchange(a, 1) for a in arrays]]
    return tuple(finish(entries, total, other, squares, bases, masters, old, blocks))


def solution(mesh):
    z_count = mesh.shape["fs"] // CORES
    tp_count = mesh.shape["tp"]
    short = z_count == 4 and tp_count == 4
    return jax.shard_map(
        short_body if short else plain_body,
        mesh=mesh,
        in_specs=(P(("fs", "tp"), None),) * 4 + (P(),) * 2 + (P("fs", "tp"),) * 6,
        out_specs=(P("fs", "tp"),) * 8 + (P(None, "tp"),) * 2,
        check_vma=False,
    )
```

```python
import jax
import jax.numpy as jnp
from jax import lax
from jax.experimental import pallas as pl
from jax.experimental.pallas import tpu as pltpu
from jax.sharding import PartitionSpec as P


CORES = 2


def low_term(saved, cotangent, basis):
    reduced = jnp.dot(saved, basis, preferred_element_type=jnp.float32).astype(jnp.bfloat16)
    return lax.dot_general(
        reduced, cotangent, (((0,), (0,)), ((), ())), preferred_element_type=jnp.float32
    )


def moments(first, second, grad):
    first_new = 0.8 * first + 0.2 * grad
    second_new = 0.9 * second + 0.1 * grad * grad
    return (first_new, second_new, first_new / (jnp.sqrt(second_new) + 1e-08))


def weight_step(basis, direction, fs_count):
    row_count = basis.shape[0] // fs_count
    rows_here = lax.dynamic_slice_in_dim(basis, lax.axis_index("fs") * row_count, row_count, 0)
    return -jnp.dot(rows_here.astype(jnp.float32), direction, precision=lax.Precision.HIGHEST)


def clip_of(squares, entries):
    return jnp.minimum(1.0, 1.0 / jnp.sqrt(squares / entries + 1e-06))


def plain_body(
    in_saved,
    in_cotangent,
    point_saved,
    point_cotangent,
    in_basis,
    point_basis,
    in_first,
    in_second,
    point_first,
    point_second,
    in_master,
    point_master,
):
    fs_count = lax.axis_size("fs")
    in_low = low_term(in_saved, in_cotangent, in_basis)
    point_low = low_term(point_saved, point_cotangent, point_basis)
    rank_rows = in_low.shape[0]
    entries = 1.0 * rank_rows * (in_low.shape[1] + point_low.shape[1])
    part_in, part_point = (
        lax.psum_scatter(in_low, "tp", scatter_dimension=1, tiled=True),
        lax.psum_scatter(point_low, "tp", scatter_dimension=1, tiled=True),
    )
    sum_in, sum_point = lax.psum((part_in, part_point), "fs")
    squares = lax.psum(jnp.sum(sum_in * sum_in) + jnp.sum(sum_point * sum_point), "tp")
    clip_factor = clip_of(squares, entries)
    previous = tuple(
        lax.all_gather(a, "fs", axis=0, tiled=True)
        for a in (in_first, in_second, point_first, point_second)
    )
    in_first_all, in_second_all, in_direction = moments(
        previous[0], previous[1], clip_factor * sum_in
    )
    point_first_all, point_second_all, point_direction = moments(
        previous[2], previous[3], clip_factor * sum_point
    )
    row_count = rank_rows // fs_count
    row_start = lax.axis_index("fs") * row_count
    mine = tuple(
        lax.dynamic_slice_in_dim(a, row_start, row_count, 0)
        for a in (in_first_all, in_second_all, point_first_all, point_second_all)
    )
    in_step = weight_step(in_basis, in_direction, fs_count)
    point_step = weight_step(point_basis, point_direction, fs_count)
    in_master_new = in_master + in_step
    point_master_new = point_master + point_step
    in_copy, point_copy = (
        lax.all_gather(in_master_new.astype(jnp.bfloat16), "fs", axis=0, tiled=True),
        lax.all_gather(point_master_new.astype(jnp.bfloat16), "fs", axis=0, tiled=True),
    )
    return (*mine, in_step, point_step, in_master_new, point_master_new, in_copy, point_copy)


def exchange(x, fs_mask, tp_mask=0):
    fs_count, tp_count = lax.axis_size("fs"), lax.axis_size("tp")
    pairs = [
        (f * tp_count + t, (f ^ fs_mask) * tp_count + (t ^ tp_mask))
        for f in range(fs_count)
        for t in range(tp_count)
    ]
    return lax.ppermute(x, ("fs", "tp"), pairs)


PLAIN_UNIT = 2.0**-14
VMEM = pl.BlockSpec(memory_space=pltpu.VMEM)
HBM = pl.BlockSpec(memory_space=pltpu.HBM)
TAG = 8
PIECES = 4
CUTS = (5,)


def shape(*dims, dtype=jnp.float32):
    return jax.ShapeDtypeStruct(dims, dtype)


def code(y):
    y2 = y * y
    y4 = y2 * y2
    y8 = y4 * y4
    return jnp.where(y < 0.0, -y8, y8).astype(jnp.bfloat16)


def uncode(t):
    t = t.astype(jnp.float32)
    size = jnp.exp2(jnp.log2(jnp.abs(t)) * 0.125)
    return jnp.where(t < 0.0, -size, size)


def unit_for(largest):
    unit = jnp.maximum(largest, 1e-30) * (1.0156 * 2.0**-15.75)
    return unit.astype(jnp.bfloat16)


def call(kernel, outs, args, mib, hbm_args=False, hbm_outs=False, scratch=()):
    return pl.pallas_call(
        kernel,
        out_shape=outs,
        in_specs=[HBM if hbm_args else VMEM] * len(args),
        out_specs=[HBM if hbm_outs else VMEM] * len(outs),
        scratch_shapes=scratch,
        compiler_params=pltpu.CompilerParams(vmem_limit_bytes=mib << 20),
    )(*args)


def in_hbm(arrays):
    return [pltpu.with_memory_space_constraint(a, pltpu.HBM) for a in arrays]


def pack(stored, cuts):
    cols = stored[0].shape[1]
    packed = sum(a.shape[0] for a in stored)
    count = len(stored)
    edges = [0, *cuts, packed]

    def kernel(*refs):
        sources, outs = refs[:count], refs[count : count + len(edges)]
        held, sems = refs[count + len(edges) : -1], refs[-1]
        copies = [
            pltpu.make_async_copy(src, dst, sems.at[n])
            for n, (src, dst) in enumerate(zip(sources, held))
        ]
        for copy in copies:
            copy.start()
        row = 0
        for n in range(count):
            copies[n].wait()
            size = held[n].shape[0]
            value = code(held[n][...] * (1.0 / PLAIN_UNIT))
            outs[0][row : row + size, :] = value
            for part, low, high in zip(outs[1:], edges, edges[1:]):
                first, last = max(low, row), min(high, row + size)
                if first < last:
                    part[first - low : last - low, :] = value[first - row : last - row, :]
            row += size

    scratch = [pltpu.VMEM(a.shape, a.dtype) for a in stored]
    scratch += [pltpu.SemaphoreType.DMA((count,))]
    sizes = [packed] + [high - low for low, high in zip(edges, edges[1:])]
    outs = [shape(n, cols, dtype=jnp.bfloat16) for n in sizes]
    return call(kernel, outs, in_hbm(stored), 6, hbm_args=True, scratch=scratch)


def low_terms(saved, cotangents, bases):
    rank, width = bases[0].shape[1], cotangents[0].shape[1]
    arrays = (bases[0], saved[0], bases[1], saved[1], *cotangents)
    count = len(arrays)

    def kernel(*refs):
        sources, (give, keep) = refs[:count], refs[count : count + 2]
        held, sems = refs[count + 2 : 2 * count + 2], refs[2 * count + 2]
        core = lax.axis_index("fs") % CORES
        copies = [
            pltpu.make_async_copy(src, dst, sems.at[n])
            for n, (src, dst) in enumerate(zip(sources, held))
        ]
        for copy in copies:
            copy.start()
        reduced = []
        for which in range(2):
            copies[2 * which].wait()
            copies[2 * which + 1].wait()
            value = jnp.dot(
                held[2 * which + 1][...], held[2 * which][...], preferred_element_type=jnp.float32
            )
            reduced.append(value.astype(jnp.bfloat16))
        for which in range(2):
            copies[4 + which].wait()
            term = lax.dot_general(
                reduced[which],
                held[4 + which][...],
                (((0,), (0,)), ((), ())),
                preferred_element_type=jnp.float32,
            )

            @pl.when(core == which)
            def _():
                keep[...] = term

            @pl.when(core != which)
            def _():
                give[...] = term

    scratch = [pltpu.VMEM(a.shape, a.dtype) for a in arrays]
    scratch += [pltpu.SemaphoreType.DMA((count,))]
    outs = [shape(rank, width)] * 2
    return call(kernel, outs, in_hbm(arrays), 12, hbm_args=True, scratch=scratch)


def put_coded(ref, value, unit):
    rank = value.shape[0]
    ref[:rank, :] = code(value * (1.0 / unit.astype(jnp.float32)))
    ref[rank:, :] = jnp.full((TAG, ref.shape[1]), unit, jnp.bfloat16)


def get_coded(ref):
    rank = ref.shape[0] - TAG
    return uncode(ref[:rank, :]) * ref[rank:, :].astype(jnp.float32)[:1, :1]


def chip_sum(keep, given, count):
    rank, width = keep.shape
    cols = width // count

    def kernel(keep, given, mine, *rest):
        coded, total = rest[:-1], rest[-1]
        column = lax.axis_index("tp")
        value = keep[...] + given[...]
        total[...] = value
        unit = unit_for(jnp.max(jnp.abs(value)))
        mine[...] = total[:, pl.ds(pl.multiple_of(column * cols, cols), cols)]
        for k in range(1, count):
            at = pl.multiple_of((column ^ k) * cols, cols)
            put_coded(coded[k - 1], total[:, pl.ds(at, cols)], unit)

    outs = [shape(rank, cols)] + [shape(rank + TAG, cols, dtype=jnp.bfloat16)] * (count - 1)
    scratch = [pltpu.VMEM((rank, width), jnp.float32)]
    return call(kernel, outs, (keep, given), 8, scratch=scratch)


def plane_sum(mine, got):
    def kernel(mine, *refs):
        value = mine[...]
        for ref in refs[:-1]:
            value = value + get_coded(ref)
        put_coded(refs[-1], value, unit_for(jnp.max(jnp.abs(value))))

    outs = [shape(mine.shape[0] + TAG, mine.shape[1], dtype=jnp.bfloat16)]
    return call(kernel, outs, (mine, *got), 8)[0]


def pair_sum(a, b, last):
    def kernel(a, b, out, *rest):
        value = get_coded(a) + get_coded(b)
        if last:
            out[...] = value
            rest[0][...] = jnp.full(rest[0].shape, jnp.sum(value * value), jnp.float32)
        else:
            put_coded(out, value, unit_for(jnp.max(jnp.abs(value))))

    rows, cols = a.shape
    if last:
        return call(kernel, [shape(rows - TAG, cols), shape(8, 128)], (a, b), 8)
    return call(kernel, [shape(rows, cols, dtype=a.dtype)], (a, b), 8)[0]


def add_squares(parts):
    def kernel(*refs):
        value = refs[0][...]
        for ref in refs[1:-1]:
            value = value + ref[...]
        refs[-1][...] = value

    return call(kernel, [shape(*parts[0].shape)], parts, 4)[0]


def finish(entries, total, other, squares, bases, masters, old, blocks):
    rows, cols = masters[0].shape
    full, rank = bases[0].shape
    here = old[0].shape[0]
    n_sq, n_bl = len(squares), len(blocks)
    flat = [a for block in blocks for a in block]

    def spans(n, row, size):
        found, edge = [], 0
        for a in blocks[n]:
            first, last = max(edge, row), min(edge + a.shape[0], row + size)
            if first < last:
                found.append((first - row, last - first))
            edge += a.shape[0]
        return found

    def kernel(*refs):
        refs = list(refs)

        def take(n):
            part = refs[:n]
            del refs[:n]
            return part

        total, other = take(2)
        square_refs = take(n_sq)
        basis_refs = take(2)
        master_refs = take(2)
        old_refs = take(4)
        block_refs = [take(len(block)) for block in blocks]
        outs = take(10)
        grads, direction, small, own, stage, sems = refs
        me = lax.axis_index("fs")
        core = me % CORES
        copies = []

        def send(src, dst):
            copies.append(pltpu.make_async_copy(src, dst, sems.at[len(copies)]))
            copies[-1].start()

        def packed(n, row, size):
            for ref in block_refs[n]:
                if row < ref.shape[0]:
                    return uncode(ref[row : row + size, :]) * PLAIN_UNIT
                row -= ref.shape[0]

        squares = square_refs[0][...]
        for ref in square_refs[1:]:
            squares = squares + ref[...]
        clip = clip_of(squares[:1, :1], entries)
        mine = total[...] * clip
        theirs = other[...] * clip
        grads[0] = jnp.where(core == 0, mine, theirs)
        grads[1] = jnp.where(core == 0, theirs, mine)
        for which in range(2):
            for n in range(n_bl):
                at = pl.multiple_of((me ^ n) * here, here)
                first = packed(n, 2 * which * here, here)
                second = packed(n, (2 * which + 1) * here, here)
                value = moments(first, second, grads[which, pl.ds(at, here), :])[2]
                high = value.astype(jnp.bfloat16)
                direction[which, pl.ds(at, here), :] = high
                direction[which, pl.ds(pl.multiple_of(rank + at, here), here), :] = (
                    value - high.astype(jnp.float32)
                ).astype(jnp.bfloat16)
            for n in range(n_bl):
                row0 = pl.multiple_of((me ^ n) * rows, rows)
                b = basis_refs[which][pl.ds(row0, rows), :]
                both = jnp.concatenate([b, b], axis=1)
                down = jnp.dot(both, direction[which], preferred_element_type=jnp.float32)
                if n == 0:
                    own[which] = -down
                    own[2 + which] = master_refs[which][...] - down
                for first, size in spans(n, 4 * here + which * rows, rows):
                    value = packed(n, 4 * here + which * rows + first, size)
                    at = slice(first, first + size)
                    stage[2 * n + which, at, :] = (value - down[at, :]).astype(jnp.bfloat16)
                if n == 0:
                    for j in (which, 2 + which):
                        send(own.at[j], outs[4 + j])
                send(stage.at[2 * n + which], outs[8 + which].at[pl.ds(row0, rows), :])
        for which in range(2):
            grad = grads[which, pl.ds(pl.multiple_of(me * here, here), here), :]
            new = moments(old_refs[2 * which][...], old_refs[2 * which + 1][...], grad)
            for j in range(2):
                small[2 * which + j] = new[j]
                send(small.at[2 * which + j], outs[2 * which + j])
        for copy in copies:
            copy.wait()

    outs = [shape(here, cols)] * 4 + [shape(rows, cols)] * 4
    outs += [shape(full, cols, dtype=jnp.bfloat16)] * 2
    args = (total, other, *squares, *bases, *masters, *old, *flat)
    scratch = [
        pltpu.VMEM((2, rank, cols), jnp.float32),
        pltpu.VMEM((2, 2 * rank, cols), jnp.bfloat16),
        pltpu.VMEM((4, here, cols), jnp.float32),
        pltpu.VMEM((4, rows, cols), jnp.float32),
        pltpu.VMEM((2 * n_bl, rows, cols), jnp.bfloat16),
        pltpu.SemaphoreType.DMA((8 + 2 * n_bl,)),
    ]
    return call(kernel, outs, args, 24, hbm_outs=True, scratch=scratch)


def short_body(
    in_saved,
    in_cotangent,
    point_saved,
    point_cotangent,
    in_basis,
    point_basis,
    in_first,
    in_second,
    point_first,
    point_second,
    in_master,
    point_master,
):
    tp_count = lax.axis_size("tp")
    rank = in_basis.shape[1]
    entries = 1.0 * rank * (in_cotangent.shape[1] + point_cotangent.shape[1])
    masters = (in_master, point_master)
    old = (in_first, in_second, point_first, point_second)
    bases = (in_basis, point_basis)

    piece = in_master.shape[0] // PIECES
    at = [len(old) * in_first.shape[0] + n * piece for n in CUTS]
    whole, *parts = pack((*old, *masters), at)
    one = exchange(whole, CORES)
    three = [exchange(p, 3 * CORES) for p in parts]

    give, keep = low_terms(
        (in_saved, point_saved), (in_cotangent, point_cotangent), bases
    )
    given = exchange(give, 1)
    mine, *coded = chip_sum(keep, given, tp_count)
    got = [exchange(coded[k - 1], 0, k) for k in range(1, tp_count)]
    coded = plane_sum(mine, got)
    coded = pair_sum(coded, exchange(coded, CORES), False)
    total, squares = pair_sum(coded, exchange(coded, 2 * CORES), True)
    two = [exchange(t, CORES) for t in three]

    other = exchange(total, 1)
    got = [exchange(squares, 0, k) for k in range(1, tp_count)]
    squares = add_squares((squares, *got))
    squares = (squares, exchange(squares, 1))
    blocks = [[whole], [exchange(whole, 1)], [one], [exchange(one, 1)]]
    for arrays in (two, three):
        blocks += [arrays, [exchange(a, 1) for a in arrays]]
    return tuple(finish(entries, total, other, squares, bases, masters, old, blocks))


def solution(mesh):
    z_count = mesh.shape["fs"] // CORES
    tp_count = mesh.shape["tp"]
    short = z_count == 4 and tp_count == 4
    return jax.shard_map(
        short_body if short else plain_body,
        mesh=mesh,
        in_specs=(P(("fs", "tp"), None),) * 4 + (P(),) * 2 + (P("fs", "tp"),) * 6,
        out_specs=(P("fs", "tp"),) * 8 + (P(None, "tp"),) * 2,
        check_vma=False,
    )
```
